32 devices in a mesh: fs: 4 (over z), rep: 4 (over y, x), tp: 2 (over core).
Axes of the slice: x: 2, y: 2, z: 4, core: 2. Of those that a mesh axis runs over, the one named last changes fastest.
Arguments:
- normed_input: bfloat16 [2048, 1024], P(('fs', 'rep')), may hold values from -6 to 6
- query_cotangent: bfloat16 [2048, 512], P(('fs', 'rep'), 'tp'), may hold values from -0.029907227 to 0.029907227
- value_cotangent: bfloat16 [2048, 1024], P(('fs', 'rep'), 'tp'), may hold values from -0.029907227 to 0.029907227
- query_basis: bfloat16 [1024, 128], replicated, may hold values from -0.1875 to 0.1875
- value_basis: bfloat16 [1024, 128], replicated, may hold values from -0.1875 to 0.1875
- query_weight: float32 [1024, 512], P(('fs', 'rep'), 'tp'), may hold values from -0.1875 to 0.1875
- value_weight: float32 [1024, 1024], P(('fs', 'rep'), 'tp'), may hold values from -0.1875 to 0.1875
- query_first: float32 [128, 512], P(('fs', 'rep'), 'tp'), may hold values from -6 to 6
- query_second: float32 [128, 512], P(('fs', 'rep'), 'tp'), may hold values from 0.25 to 4
- value_first: float32 [128, 1024], P(('fs', 'rep'), 'tp'), may hold values from -6 to 6
- value_second: float32 [128, 1024], P(('fs', 'rep'), 'tp'), may hold values from 0.25 to 4
Outputs:
- query_update: float32 [1024, 512], P(('fs', 'rep'), 'tp')
- value_update: float32 [1024, 1024], P(('fs', 'rep'), 'tp')
- query_weight_new: float32 [1024, 512], P(('fs', 'rep'), 'tp')
- value_weight_new: float32 [1024, 1024], P(('fs', 'rep'), 'tp')
- query_first_new: float32 [128, 512], P(('fs', 'rep'), 'tp')
- query_second_new: float32 [128, 512], P(('fs', 'rep'), 'tp')
- value_first_new: float32 [128, 1024], P(('fs', 'rep'), 'tp')
- value_second_new: float32 [128, 1024], P(('fs', 'rep'), 'tp')
- query_copy: bfloat16 [1024, 512], P(None, 'tp')
- value_copy: bfloat16 [1024, 1024], P(None, 'tp')
The draws below stay inside these ranges and needn't reach their ends.
All inputs are finite; a program needn't handle non-finite values.
Results may differ from the reference program's by a relative error of at most 0.001.
Values may be sent and summed in bfloat16 or wider, within the bound.
A program may use at most 64 MiB of HBM per device.

```python
import math
import jax
import jax.numpy as jnp
from jax import lax

D = 1024
RANK = 128
QW = 512
VW = 1024
TOKENS = 2048


def block_levels(stream_key, shape, shards, smallest, top_value):
    gain = 1.0
    for dim, parts in shards:
        steps = jax.random.uniform(jax.random.fold_in(jax.random.fold_in(stream_key, 6), dim), (parts,), jnp.float32, smallest / len(shards), top_value / len(shards))
        gain = gain * jnp.repeat(jnp.exp(steps), shape[dim] // parts).reshape((-1,) + (1,) * (len(shape) - 1 - dim))
    return gain


def normal_values(key, extent, width, most, split=(), dtype=jnp.bfloat16):
    values = jax.random.normal(key, extent, jnp.float32) * width
    if len(split) > 0:
        values = block_levels(key, extent, split, -0.22, 0.18) * values
    return jnp.clip(values, min=-most, max=most).astype(dtype)


def setup_inputs(seed: int = 0) -> dict:
    arg_keys = jax.random.split(jax.random.key(seed), 12)
    normed_input = normal_values(arg_keys[0], (TOKENS, D), 1.0, 6.0, ((0, 16),))
    query_cotangent = normal_values(arg_keys[1], (TOKENS, QW), 0.005, 0.029907227, ((0, 16), (1, 2)))
    value_cotangent = normal_values(arg_keys[2], (TOKENS, VW), 0.005, 0.029907227, ((0, 16), (1, 2)))
    query_basis = normal_values(arg_keys[3], (D, RANK), D ** -0.5, 0.1875)
    value_basis = normal_values(arg_keys[4], (D, RANK), D ** -0.5, 0.1875)
    query_weight = normal_values(arg_keys[5], (D, QW), D ** -0.5, 0.1875, ((0, 16), (1, 2)), jnp.float32)
    value_weight = normal_values(arg_keys[6], (D, VW), D ** -0.5, 0.1875, ((0, 16), (1, 2)), jnp.float32)
    query_first = normal_values(arg_keys[7], (RANK, QW), 1.0, 6.0, ((0, 16), (1, 2)), jnp.float32)
    query_second = jnp.clip(jnp.exp(math.log(4.0) - 2.7725887 * jax.random.uniform(arg_keys[8], (RANK, QW), jnp.float32) ** block_levels(arg_keys[8], (RANK, QW), ((0, 16), (1, 2)), -0.2, 0.2)), 0.25, 4.0)
    value_first = normal_values(arg_keys[9], (RANK, VW), 1.0, 6.0, ((0, 16), (1, 2)), jnp.float32)
    value_second = jnp.clip(jnp.exp(math.log(4.0) - 2.7725887 * jax.random.uniform(arg_keys[10], (RANK, VW), jnp.float32) ** block_levels(arg_keys[10], (RANK, VW), ((0, 16), (1, 2)), -0.2, 0.2)), 0.25, 4.0)
    return dict(normed_input=normed_input, query_cotangent=query_cotangent, value_cotangent=value_cotangent, query_basis=query_basis, value_basis=value_basis, query_weight=query_weight, value_weight=value_weight, query_first=query_first, query_second=query_second, value_first=value_first, value_second=value_second)


def update_matrix(normed_input, cotangent, basis, weight, first_old, second_old):
    gradient = jnp.dot(normed_input.T, cotangent, preferred_element_type=jnp.float32)
    basis_wide = basis.astype(jnp.float32)
    projected = jnp.dot(basis_wide.T, gradient, precision=lax.Precision.HIGHEST)
    first_new = 0.9 * first_old + 0.1 * projected
    second_new = 0.99 * second_old + 0.01 * projected * projected
    direction = first_new / (jnp.sqrt(second_new) + 1e-08)
    norm_scale = jnp.sqrt(jnp.mean(direction * direction) + 1.0)
    update = jnp.dot(basis_wide, direction, precision=lax.Precision.HIGHEST) / norm_scale
    weight_new = weight - 0.01 * update
    return (update, weight_new, first_new, second_new, weight_new.astype(jnp.bfloat16))

def reference(normed_input, query_cotangent, value_cotangent, query_basis, value_basis, query_weight, value_weight, query_first, query_second, value_first, value_second):
    query_out = update_matrix(normed_input, query_cotangent, query_basis, query_weight, query_first, query_second)
    value_out = update_matrix(normed_input, value_cotangent, value_basis, value_weight, value_first, value_second)
    return (query_out[0], value_out[0], query_out[1], value_out[1], query_out[2], query_out[3], value_out[2], value_out[3], query_out[4], value_out[4])
```

```python
import functools
import jax
import jax.numpy as jnp
from jax import lax
from jax.experimental import pallas as pl
from jax.experimental.pallas import tpu as pltpu
from jax.sharding import PartitionSpec as P


def moments(projected, first_old, second_old):
    first_new = 0.9 * first_old + 0.1 * projected
    second_new = 0.99 * second_old + 0.01 * projected * projected
    return (first_new, second_new, first_new / (jnp.sqrt(second_new) + 1e-08))


def finish(whole_dir, basis_rows, weight, squares, entries):
    norm_scale = jnp.sqrt(squares / entries + 1.0)
    update = jnp.dot(basis_rows, whole_dir, precision=lax.Precision.HIGHEST) / norm_scale
    weight_new = weight - 0.01 * update
    return (update, weight_new, weight_new.astype(jnp.bfloat16))


def split_parts(reduced):
    high_part = reduced.astype(jnp.bfloat16)
    held = lax.optimization_barrier(high_part)
    low_part = (reduced - held.astype(jnp.float32)).astype(jnp.bfloat16)
    return (high_part, low_part)


def parts_product(high_part, low_part, cotangent):
    dims = (((0,), (0,)), ((), ()))
    first_term = lax.dot_general(high_part, cotangent, dims, preferred_element_type=jnp.float32)
    second_term = lax.dot_general(low_part, cotangent, dims, preferred_element_type=jnp.float32)
    return first_term + second_term


def body(
    normed_input,
    query_cotangent,
    value_cotangent,
    query_basis,
    value_basis,
    query_weight,
    value_weight,
    query_first,
    query_second,
    value_first,
    value_second,
):
    row_count = query_weight.shape[0]
    query_width = query_cotangent.shape[1]
    offset = lax.axis_index(("fs", "rep")) * row_count
    query_rows = lax.dynamic_slice_in_dim(query_basis, offset, row_count, 0).astype(jnp.float32)
    value_rows = lax.dynamic_slice_in_dim(value_basis, offset, row_count, 0).astype(jnp.float32)
    reduced_query = jnp.dot(normed_input, query_basis, preferred_element_type=jnp.float32)
    reduced_value = jnp.dot(normed_input, value_basis, preferred_element_type=jnp.float32)
    query_high, query_low = split_parts(reduced_query)
    value_high, value_low = split_parts(reduced_value)
    projected = lax.psum_scatter(
        jnp.concatenate(
            [
                parts_product(query_high, query_low, query_cotangent),
                parts_product(value_high, value_low, value_cotangent),
            ],
            axis=1,
        ),
        ("fs", "rep"),
        scatter_dimension=0,
        tiled=True,
    )
    query_projected = projected[:, :query_width]
    value_projected = projected[:, query_width:]
    query_first_new, query_second_new, query_dir = moments(
        query_projected, query_first, query_second
    )
    value_first_new, value_second_new, value_dir = moments(
        value_projected, value_first, value_second
    )
    query_whole, value_whole = (
        lax.all_gather(query_dir, ("fs", "rep"), axis=0, tiled=True),
        lax.all_gather(value_dir, ("fs", "rep"), axis=0, tiled=True),
    )
    query_squares, value_squares = lax.psum(
        (jnp.sum(query_dir * query_dir), jnp.sum(value_dir * value_dir)), ("fs", "rep", "tp")
    )
    tp_count = lax.axis_size("tp")
    query_update, query_weight_new, query_half = finish(
        query_whole,
        query_rows,
        query_weight,
        query_squares,
        query_whole.shape[0] * query_whole.shape[1] * tp_count,
    )
    value_update, value_weight_new, value_half = finish(
        value_whole,
        value_rows,
        value_weight,
        value_squares,
        value_whole.shape[0] * value_whole.shape[1] * tp_count,
    )
    query_copy, value_copy = (
        lax.all_gather(query_half, ("fs", "rep"), axis=0, tiled=True),
        lax.all_gather(value_half, ("fs", "rep"), axis=0, tiled=True),
    )
    return (
        query_update,
        value_update,
        query_weight_new,
        value_weight_new,
        query_first_new,
        query_second_new,
        value_first_new,
        value_second_new,
        query_copy,
        value_copy,
    )


MESH = pl.DeviceIdType.MESH
f32, bf16 = jnp.float32, jnp.bfloat16


def two_parts(x):
    high = x.astype(bf16)
    return high, (x - high.astype(f32)).astype(bf16)


def three_parts(x):
    high = x.astype(bf16)
    rest = x - high.astype(f32)
    middle = rest.astype(bf16)
    return high, middle, (rest - middle.astype(f32)).astype(bf16)


def remote(src, dst, sems, index, peer):
    return pltpu.make_async_remote_copy(
        src_ref=src,
        dst_ref=dst,
        send_sem=sems[0].at[index],
        recv_sem=sems[1].at[index],
        device_id=peer,
        device_id_type=MESH,
    )


def kernel(
    F, R, T,
    x_ref, qc_ref, vc_ref, qb_ref, vb_ref, qw_ref, vw_ref, qf_ref, qs_ref, vf_ref, vs_ref,
    qu_ref, vu_ref, qn_ref, vn_ref, qfn_ref, qsn_ref, vfn_ref, vsn_ref, qcopy_ref, vcopy_ref,
    part, got1, mid, got2, dirs, squares, squares_in,
    s1, r1, s2, r2, s3, r3, s4, r4, s5, r5, s6, r6, s7, r7,
):
    z, r, t = lax.axis_index("fs"), lax.axis_index("rep"), lax.axis_index("tp")
    zs = [lax.rem(z + k, F) for k in range(F)]
    rs = [lax.rem(r + k, R) for k in range(R)]
    ts = [lax.rem(t + k, T) for k in range(T)]
    back = [lax.rem(z + F - k, F) for k in range(F)]
    rows = qw_ref.shape[0]
    QC, VC = qc_ref.shape[1], vc_ref.shape[1]
    M = qf_ref.shape[0]

    barrier = pltpu.get_barrier_semaphore()
    for axis, others in (("rep", rs), ("fs", zs), ("tp", ts)):
        for other in others[1:]:
            pl.semaphore_signal(barrier, inc=1, device_id={axis: other}, device_id_type=MESH)

    x = x_ref[...]
    for basis, cot, start, width in ((qb_ref, qc_ref, 0, QC), (vb_ref, vc_ref, QC, VC)):
        reduced = jnp.dot(x, basis[...], preferred_element_type=f32).T
        high, low = two_parts(reduced)
        c = cot[...]
        total = jnp.dot(high, c, preferred_element_type=f32) + jnp.dot(
            low, c, preferred_element_type=f32
        )
        for a in range(F):
            for b in range(R):
                at = (a * R + b) * M
                part[b, a, :, start : start + width] = total[at : at + M]

    pl.semaphore_wait(barrier, F + R + T - 3)

    sends = []
    first = [remote(part.at[rs[k]], got1.at[k], (s1, r1), k, {"rep": rs[k]}) for k in range(1, R)]
    for c in first:
        c.start()
    sends += first
    for c in first:
        c.wait_recv()
    total = part[r]
    for k in range(1, R):
        total = total + got1[k]
    mid[...] = total
    second = [remote(mid.at[zs[k]], got2.at[k], (s2, r2), k, {"fs": zs[k]}) for k in range(1, F)]
    for c in second:
        c.start()
    sends += second
    projected = mid[z]
    for k in range(1, F):
        second[k - 1].wait_recv()
        projected = projected + got2[k]

    for f_ref, s_ref, fn_ref, sn_ref, start, width in (
        (qf_ref, qs_ref, qfn_ref, qsn_ref, 0, QC),
        (vf_ref, vs_ref, vfn_ref, vsn_ref, QC, VC),
    ):
        p = projected[:, start : start + width]
        fn = 0.9 * f_ref[...] + 0.1 * p
        sn = 0.99 * s_ref[...] + 0.01 * p * p
        fn_ref[...] = fn
        sn_ref[...] = sn
        dirs[z, r, :, start : start + width] = fn / (jnp.sqrt(sn) + 1e-08)

    third = [remote(dirs.at[z, r], dirs.at[z, r], (s3, r3), k, {"fs": zs[k]}) for k in range(1, F)]
    for c in third:
        c.start()
    sends += third
    fourth = []
    for j in range(F):
        if j > 0:
            third[j - 1].wait_recv()
        block = dirs.at[back[j], r]
        for k in range(1, R):
            c = remote(block, block, (s4, r4), (j, k), {"rep": rs[k]})
            c.start()
            fourth.append(c)
    sends += fourth
    for c in fourth:
        c.wait_recv()

    whole = dirs[...].reshape(F * R * M, QC + VC)
    for i, (start, width) in enumerate(((0, QC), (QC, VC))):
        d = whole[:, start : start + width]
        d = (d * d).reshape(F * R * M // 8, 8, width).sum(axis=0)
        acc = d[:, :128]
        for b in range(1, width // 128):
            acc = acc + d[:, b * 128 : (b + 1) * 128]
        squares[i] = acc
    fifth = [remote(squares, squares_in.at[k], (s5, r5), k, {"tp": ts[k]}) for k in range(1, T)]
    for c in fifth:
        c.start()
    sends += fifth

    offset = pl.multiple_of((z * R + r) * rows, rows)
    raw = []
    for basis, start, width in ((qb_ref, 0, QC), (vb_ref, QC, VC)):
        b = basis[pl.ds(offset, rows), :]
        d1, d2, d3 = three_parts(whole[:, start : start + width])
        raw.append(
            jnp.dot(b, d1, preferred_element_type=f32)
            + (jnp.dot(b, d2, preferred_element_type=f32) + jnp.dot(b, d3, preferred_element_type=f32))
        )
    for c in fifth:
        c.wait_recv()
    sq = squares[...]
    for k in range(1, T):
        sq = sq + squares_in[k]
    for i, (w_ref, u_ref, n_ref, copy_ref, width) in enumerate((
        (qw_ref, qu_ref, qn_ref, qcopy_ref, QC),
        (vw_ref, vu_ref, vn_ref, vcopy_ref, VC),
    )):
        scale = jnp.sqrt(jnp.sum(sq[i], keepdims=True) / (F * R * M * width * T) + 1.0)
        update = raw[i] / scale
        new = w_ref[...] - 0.01 * update
        u_ref[...] = update
        n_ref[...] = new
        copy_ref[pl.ds(offset, rows), :] = new.astype(bf16)

    sixth = []
    for k in range(1, F):
        for i, ref in enumerate((qcopy_ref, vcopy_ref)):
            own = ref.at[pl.ds(offset, rows), :]
            c = remote(own, own, (s6, r6), (k, i), {"fs": zs[k]})
            c.start()
            sixth.append(c)
    sends += sixth
    seventh = []
    for j in range(F):
        at = pl.multiple_of((back[j] * R + r) * rows, rows)
        for i, ref in enumerate((qcopy_ref, vcopy_ref)):
            if j > 0:
                sixth[(j - 1) * 2 + i].wait_recv()
            block = ref.at[pl.ds(at, rows), :]
            for k in range(1, R):
                c = remote(block, block, (s7, r7), (j, k * 2 + i), {"rep": rs[k]})
                c.start()
                seventh.append(c)
    sends += seventh
    for c in seventh:
        c.wait_recv()
    for c in sends:
        c.wait_send()


def fused(plain, *args):
    x, qc, vc, qb, vb, qw, vw, qf, qs, vf, vs = args
    F, R, T = (lax.axis_size(name) for name in ("fs", "rep", "tp"))
    QC, VC = qc.shape[1], vc.shape[1]
    M, rows = qf.shape[0], qw.shape[0]
    aligned = M % 8 == 0 and rows % 16 == 0 and QC % 128 == 0 and VC % 128 == 0
    if not aligned:
        return plain(*args)
    W = QC + VC
    out = jax.ShapeDtypeStruct
    vmem = pl.BlockSpec(memory_space=pltpu.VMEM)
    dma = pltpu.SemaphoreType.DMA
    return tuple(
        pl.pallas_call(
            functools.partial(kernel, F, R, T),
            out_shape=[
                out(qw.shape, f32),
                out(vw.shape, f32),
                out(qw.shape, f32),
                out(vw.shape, f32),
                out(qf.shape, f32),
                out(qf.shape, f32),
                out(vf.shape, f32),
                out(vf.shape, f32),
                out((rows * F * R, QC), bf16),
                out((rows * F * R, VC), bf16),
            ],
            in_specs=[vmem] * 11,
            out_specs=[vmem] * 10,
            scratch_shapes=[
                pltpu.VMEM((R, F, M, W), f32),
                pltpu.VMEM((R, F, M, W), f32),
                pltpu.VMEM((F, M, W), f32),
                pltpu.VMEM((F, M, W), f32),
                pltpu.VMEM((F, R, M, W), f32),
                pltpu.VMEM((2, 8, 128), f32),
                pltpu.VMEM((T, 2, 8, 128), f32),
                dma((R,)), dma((R,)),
                dma((F,)), dma((F,)),
                dma((F,)), dma((F,)),
                dma((F, R)), dma((F, R)),
                dma((T,)), dma((T,)),
                dma((F, 2)), dma((F, 2)),
                dma((F, 2 * R)), dma((F, 2 * R)),
            ],
            compiler_params=pltpu.CompilerParams(
                collective_id=0, has_side_effects=True, vmem_limit_bytes=48 * 2**20
            ),
        )(*args)
    )


def solution(mesh):
    in_specs = (
        P(("fs", "rep"), None),
        P(("fs", "rep"), "tp"),
        P(("fs", "rep"), "tp"),
        P(),
        P(),
        P(("fs", "rep"), "tp"),
        P(("fs", "rep"), "tp"),
        P(("fs", "rep"), "tp"),
        P(("fs", "rep"), "tp"),
        P(("fs", "rep"), "tp"),
        P(("fs", "rep"), "tp"),
    )
    out_specs = (
        P(("fs", "rep"), "tp"),
        P(("fs", "rep"), "tp"),
        P(("fs", "rep"), "tp"),
        P(("fs", "rep"), "tp"),
        P(("fs", "rep"), "tp"),
        P(("fs", "rep"), "tp"),
        P(("fs", "rep"), "tp"),
        P(("fs", "rep"), "tp"),
        P(None, "tp"),
        P(None, "tp"),
    )
    return jax.shard_map(functools.partial(fused, body), mesh=mesh, in_specs=in_specs, out_specs=out_specs, check_vma=False)
```

```python
import functools
import jax
import jax.numpy as jnp
from jax import lax
from jax.experimental import pallas as pl
from jax.experimental.pallas import tpu as pltpu
from jax.sharding import PartitionSpec as P


def moments(projected, first_old, second_old):
    first_new = 0.9 * first_old + 0.1 * projected
    second_new = 0.99 * second_old + 0.01 * projected * projected
    return (first_new, second_new, first_new / (jnp.sqrt(second_new) + 1e-08))


def finish(whole_dir, basis_rows, weight, squares, entries):
    norm_scale = jnp.sqrt(squares / entries + 1.0)
    update = jnp.dot(basis_rows, whole_dir, precision=lax.Precision.HIGHEST) / norm_scale
    weight_new = weight - 0.01 * update
    return (update, weight_new, weight_new.astype(jnp.bfloat16))


def split_parts(reduced):
    high_part = reduced.astype(jnp.bfloat16)
    held = lax.optimization_barrier(high_part)
    low_part = (reduced - held.astype(jnp.float32)).astype(jnp.bfloat16)
    return (high_part, low_part)


def parts_product(high_part, low_part, cotangent):
    dims = (((0,), (0,)), ((), ()))
    first_term = lax.dot_general(high_part, cotangent, dims, preferred_element_type=jnp.float32)
    second_term = lax.dot_general(low_part, cotangent, dims, preferred_element_type=jnp.float32)
    return first_term + second_term


def body(
    normed_input,
    query_cotangent,
    value_cotangent,
    query_basis,
    value_basis,
    query_weight,
    value_weight,
    query_first,
    query_second,
    value_first,
    value_second,
):
    row_count = query_weight.shape[0]
    query_width = query_cotangent.shape[1]
    offset = lax.axis_index(("fs", "rep")) * row_count
    query_rows = lax.dynamic_slice_in_dim(query_basis, offset, row_count, 0).astype(jnp.float32)
    value_rows = lax.dynamic_slice_in_dim(value_basis, offset, row_count, 0).astype(jnp.float32)
    reduced_query = jnp.dot(normed_input, query_basis, preferred_element_type=jnp.float32)
    reduced_value = jnp.dot(normed_input, value_basis, preferred_element_type=jnp.float32)
    query_high, query_low = split_parts(reduced_query)
    value_high, value_low = split_parts(reduced_value)
    projected = lax.psum_scatter(
        jnp.concatenate(
            [
                parts_product(query_high, query_low, query_cotangent),
                parts_product(value_high, value_low, value_cotangent),
            ],
            axis=1,
        ),
        ("fs", "rep"),
        scatter_dimension=0,
        tiled=True,
    )
    query_projected = projected[:, :query_width]
    value_projected = projected[:, query_width:]
    query_first_new, query_second_new, query_dir = moments(
        query_projected, query_first, query_second
    )
    value_first_new, value_second_new, value_dir = moments(
        value_projected, value_first, value_second
    )
    query_whole, value_whole = (
        lax.all_gather(query_dir, ("fs", "rep"), axis=0, tiled=True),
        lax.all_gather(value_dir, ("fs", "rep"), axis=0, tiled=True),
    )
    query_squares, value_squares = lax.psum(
        (jnp.sum(query_dir * query_dir), jnp.sum(value_dir * value_dir)), ("fs", "rep", "tp")
    )
    tp_count = lax.axis_size("tp")
    query_update, query_weight_new, query_half = finish(
        query_whole,
        query_rows,
        query_weight,
        query_squares,
        query_whole.shape[0] * query_whole.shape[1] * tp_count,
    )
    value_update, value_weight_new, value_half = finish(
        value_whole,
        value_rows,
        value_weight,
        value_squares,
        value_whole.shape[0] * value_whole.shape[1] * tp_count,
    )
    query_copy, value_copy = (
        lax.all_gather(query_half, ("fs", "rep"), axis=0, tiled=True),
        lax.all_gather(value_half, ("fs", "rep"), axis=0, tiled=True),
    )
    return (
        query_update,
        value_update,
        query_weight_new,
        value_weight_new,
        query_first_new,
        query_second_new,
        value_first_new,
        value_second_new,
        query_copy,
        value_copy,
    )


MESH = pl.DeviceIdType.MESH
VMEM_LIMIT = 60 * 2**20
OUT_LIMIT = 16 * 2**20
f32, bf16 = jnp.float32, jnp.bfloat16


def two_parts(x):
    high = x.astype(bf16)
    return high, (x - high.astype(f32)).astype(bf16)


def three_parts(x):
    high = x.astype(bf16)
    rest = x - high.astype(f32)
    middle = rest.astype(bf16)
    return high, middle, (rest - middle.astype(f32)).astype(bf16)


def remote(src, dst, sems, index, peer):
    return pltpu.make_async_remote_copy(
        src_ref=src,
        dst_ref=dst,
        send_sem=sems[0].at[index],
        recv_sem=sems[1].at[index],
        device_id=peer,
        device_id_type=MESH,
    )


def kernel(
    F, R, T,
    x_hbm, qc_hbm, vc_hbm, qb_hbm, vb_hbm, qw_hbm, vw_hbm, qf_hbm, qs_hbm, vf_hbm, vs_hbm,
    u_ref, n_ref, fn_ref, sn_ref, copy_ref,
    x_ref, qc_ref, vc_ref, qb_ref, vb_ref, w_ref, f_ref, s_ref,
    part, got1, mid, got2, dirs, squares, squares_in,
    load, s1, r1, s2, r2, s3, r3, s4, r4, s5, r5, s6, r6, s7, r7,
):
    z, r, t = lax.axis_index("fs"), lax.axis_index("rep"), lax.axis_index("tp")
    zs = [lax.rem(z + k, F) for k in range(F)]
    rs = [lax.rem(r + k, R) for k in range(R)]
    ts = [lax.rem(t + k, T) for k in range(T)]
    back = [lax.rem(z + F - k, F) for k in range(F)]
    rows = qw_hbm.shape[0]
    QC, VC = qc_hbm.shape[1], vc_hbm.shape[1]
    M = qf_hbm.shape[0]

    barrier = pltpu.get_barrier_semaphore()
    for axis, others in (("rep", rs), ("fs", zs), ("tp", ts)):
        for other in others[1:]:
            pl.semaphore_signal(barrier, inc=1, device_id={axis: other}, device_id_type=MESH)

    query, value = pl.ds(0, QC), pl.ds(QC, VC)
    loads = [
        pltpu.make_async_copy(src, dst, load.at[i])
        for i, (src, dst) in enumerate((
            (x_hbm, x_ref),
            (qb_hbm, qb_ref),
            (qc_hbm, qc_ref),
            (vb_hbm, vb_ref),
            (vc_hbm, vc_ref),
            (qf_hbm, f_ref.at[:, query]),
            (vf_hbm, f_ref.at[:, value]),
            (qs_hbm, s_ref.at[:, query]),
            (vs_hbm, s_ref.at[:, value]),
            (qw_hbm, w_ref.at[:, query]),
            (vw_hbm, w_ref.at[:, value]),
        ))
    ]
    for c in loads:
        c.start()

    loads[0].wait()
    x = x_ref[...]
    for i, (basis, cot, start, width) in enumerate(
        ((qb_ref, qc_ref, 0, QC), (vb_ref, vc_ref, QC, VC))
    ):
        loads[1 + 2 * i].wait()
        loads[2 + 2 * i].wait()
        reduced = jnp.dot(x, basis[...], preferred_element_type=f32).T
        high, low = two_parts(reduced)
        c = cot[...]
        total = jnp.dot(high, c, preferred_element_type=f32) + jnp.dot(
            low, c, preferred_element_type=f32
        )
        for a in range(F):
            for b in range(R):
                at = (a * R + b) * M
                part[b, a, :, start : start + width] = total[at : at + M]

    pl.semaphore_wait(barrier, F + R + T - 3)

    sends = []
    order = list(range(1, F)) + [0]
    first = {
        (j, k): remote(
            part.at[rs[k], zs[j]], got1.at[k, j], (s1, r1), (j, k), {"rep": rs[k]}
        )
        for j in order
        for k in range(1, R)
    }
    for c in first.values():
        c.start()
    sends += list(first.values())
    second = {}
    for j in order:
        total = part[r, zs[j]]
        for k in range(1, R):
            first[j, k].wait_recv()
            total = total + got1[k, j]
        if j > 0:
            mid[j] = total
            second[j] = remote(mid.at[j], got2.at[j], (s2, r2), j, {"fs": zs[j]})
            second[j].start()
    sends += list(second.values())
    for c in loads[5:]:
        c.wait()
    projected = total
    for j in range(1, F):
        second[j].wait_recv()
        projected = projected + got2[j]

    fn = 0.9 * f_ref[...] + 0.1 * projected
    sn = 0.99 * s_ref[...] + 0.01 * projected * projected
    dirs[z, r] = fn / (jnp.sqrt(sn) + 1e-08)

    third = [remote(dirs.at[z, r], dirs.at[z, r], (s3, r3), k, {"fs": zs[k]}) for k in range(1, F)]
    for c in third:
        c.start()
    sends += third
    fourth = []
    for j in range(F):
        if j > 0:
            third[j - 1].wait_recv()
        block = dirs.at[back[j], r]
        for k in range(1, R):
            c = remote(block, block, (s4, r4), (j, k), {"rep": rs[k]})
            c.start()
            fourth.append(c)
        if j == 0:
            fn_ref[...] = fn
            sn_ref[...] = sn
    sends += fourth
    for c in fourth:
        c.wait_recv()

    whole = dirs[...].reshape(F * R * M, QC + VC)
    for i, (start, width) in enumerate(((0, QC), (QC, VC))):
        d = whole[:, start : start + width]
        d = (d * d).reshape(F * R * M // 8, 8, width).sum(axis=0)
        acc = d[:, :128]
        for b in range(1, width // 128):
            acc = acc + d[:, b * 128 : (b + 1) * 128]
        squares[i] = acc
    fifth = [remote(squares, squares_in.at[k], (s5, r5), k, {"tp": ts[k]}) for k in range(1, T)]
    for c in fifth:
        c.start()
    sends += fifth

    offset = pl.multiple_of((z * R + r) * rows, rows)
    raw = []
    for basis, start, width in ((qb_ref, 0, QC), (vb_ref, QC, VC)):
        b = basis[pl.ds(offset, rows), :]
        d1, d2, d3 = three_parts(whole[:, start : start + width])
        raw.append(
            jnp.dot(b, d1, preferred_element_type=f32)
            + (jnp.dot(b, d2, preferred_element_type=f32) + jnp.dot(b, d3, preferred_element_type=f32))
        )
    for c in fifth:
        c.wait_recv()
    sq = squares[...]
    for k in range(1, T):
        sq = sq + squares_in[k]
    for i, (start, width) in enumerate(((0, QC), (QC, VC))):
        scale = jnp.sqrt(jnp.sum(sq[i], keepdims=True) / (F * R * M * width * T) + 1.0)
        update = raw[i] / scale
        new = w_ref[:, start : start + width] - 0.01 * update
        copy_ref[pl.ds(offset, rows), start : start + width] = new.astype(bf16)
        u_ref[:, start : start + width] = update
        n_ref[:, start : start + width] = new

    own = copy_ref.at[pl.ds(offset, rows), :]
    sixth = [remote(own, own, (s6, r6), k, {"fs": zs[k]}) for k in range(1, F)]
    for c in sixth:
        c.start()
    sends += sixth

    def block_of(j, rep, first_row, count):
        at = pl.multiple_of((back[j] * R + rep) * rows + first_row, count)
        return copy_ref.at[pl.ds(at, count), :]

    last = []
    split = R == 4 and rows % 32 == 0
    if split:
        half = rows // 2
        beside = (r + 1 - 2 * lax.rem(r, 2), lax.rem(r + 2, 4))
        direct = {}

        def forward(j):
            for a in range(2):
                direct[j, a].wait_recv()
                block = block_of(j, beside[a], a * half, half)
                c = remote(block, block, (s7, r7), (j, 2 + a), {"rep": beside[1 - a]})
                c.start()
                last.append(c)

    for j in range(F):
        if j > 0:
            sixth[j - 1].wait_recv()
        block = block_of(j, r, 0, rows)
        if split:
            for a in range(2):
                direct[j, a] = remote(block, block, (s7, r7), (j, a), {"rep": beside[a]})
                direct[j, a].start()
                sends.append(direct[j, a])
            if j > 0:
                forward(j - 1)
        else:
            for k in range(1, R):
                c = remote(block, block, (s7, r7), (j, k), {"rep": rs[k]})
                c.start()
                last.append(c)
    if split:
        forward(F - 1)
    sends += last
    for c in last:
        c.wait_recv()
    for c in sends:
        c.wait_send()


def write_out(u, n, fn, sn, copy, qu, vu, qn, vn, qfn, qsn, vfn, vsn, qcopy, vcopy, sem):
    QC, VC = qu.shape[1], vu.shape[1]
    query, value = pl.ds(0, QC), pl.ds(QC, VC)
    copies = [
        pltpu.make_async_copy(src.at[:, part], dst, sem.at[i])
        for i, (src, part, dst) in enumerate((
            (copy, value, vcopy),
            (copy, query, qcopy),
            (u, value, vu),
            (n, value, vn),
            (u, query, qu),
            (n, query, qn),
            (fn, query, qfn),
            (fn, value, vfn),
            (sn, query, qsn),
            (sn, value, vsn),
        ))
    ]
    for c in copies:
        c.start()
    for c in copies:
        c.wait()


def fused(plain, *args):
    x, qc, vc, qb, vb, qw, vw, qf, qs, vf, vs = args
    F, R, T = (lax.axis_size(name) for name in ("fs", "rep", "tp"))
    QC, VC = qc.shape[1], vc.shape[1]
    M, rows = qf.shape[0], qw.shape[0]
    aligned = M % 8 == 0 and rows % 16 == 0 and QC % 128 == 0 and VC % 128 == 0
    if not aligned:
        return plain(*args)
    W = QC + VC
    out = jax.ShapeDtypeStruct
    vmem = pl.BlockSpec(memory_space=pltpu.VMEM)
    dma = pltpu.SemaphoreType.DMA
    results = pl.pallas_call(
        functools.partial(kernel, F, R, T),
        out_shape=[
            pltpu.VMEM((rows, W), f32),
            pltpu.VMEM((rows, W), f32),
            pltpu.VMEM((M, W), f32),
            pltpu.VMEM((M, W), f32),
            pltpu.VMEM((rows * F * R, W), bf16),
        ],
        in_specs=[pl.BlockSpec(memory_space=pltpu.HBM)] * 11,
        out_specs=[vmem] * 5,
        scratch_shapes=[
            pltpu.VMEM(x.shape, bf16),
            pltpu.VMEM(qc.shape, bf16),
            pltpu.VMEM(vc.shape, bf16),
            pltpu.VMEM(qb.shape, bf16),
            pltpu.VMEM(vb.shape, bf16),
            pltpu.VMEM((rows, W), f32),
            pltpu.VMEM((M, W), f32),
            pltpu.VMEM((M, W), f32),
            pltpu.VMEM((R, F, M, W), f32),
            pltpu.VMEM((R, F, M, W), f32),
            pltpu.VMEM((F, M, W), f32),
            pltpu.VMEM((F, M, W), f32),
            pltpu.VMEM((F, R, M, W), f32),
            pltpu.VMEM((2, 8, 128), f32),
            pltpu.VMEM((T, 2, 8, 128), f32),
            dma((11,)),
            dma((F, R)), dma((F, R)),
            dma((F,)), dma((F,)),
            dma((F,)), dma((F,)),
            dma((F, R)), dma((F, R)),
            dma((T,)), dma((T,)),
            dma((F,)), dma((F,)),
            dma((F, max(R, 4))), dma((F, max(R, 4))),
        ],
        compiler_params=pltpu.CompilerParams(
            collective_id=0, has_side_effects=True, vmem_limit_bytes=VMEM_LIMIT
        ),
    )(*args)
    return tuple(
        pl.pallas_call(
            write_out,
            out_shape=[
                out(qw.shape, f32),
                out(vw.shape, f32),
                out(qw.shape, f32),
                out(vw.shape, f32),
                out(qf.shape, f32),
                out(qf.shape, f32),
                out(vf.shape, f32),
                out(vf.shape, f32),
                out((rows * F * R, QC), bf16),
                out((rows * F * R, VC), bf16),
            ],
            in_specs=[vmem] * 5,
            out_specs=[pl.BlockSpec(memory_space=pltpu.HBM)] * 10,
            scratch_shapes=[dma((10,))],
            compiler_params=pltpu.CompilerParams(vmem_limit_bytes=OUT_LIMIT),
        )(*results)
    )


def solution(mesh):
    in_specs = (
        P(("fs", "rep"), None),
        P(("fs", "rep"), "tp"),
        P(("fs", "rep"), "tp"),
        P(),
        P(),
        P(("fs", "rep"), "tp"),
        P(("fs", "rep"), "tp"),
        P(("fs", "rep"), "tp"),
        P(("fs", "rep"), "tp"),
        P(("fs", "rep"), "tp"),
        P(("fs", "rep"), "tp"),
    )
    out_specs = (
        P(("fs", "rep"), "tp"),
        P(("fs", "rep"), "tp"),
        P(("fs", "rep"), "tp"),
        P(("fs", "rep"), "tp"),
        P(("fs", "rep"), "tp"),
        P(("fs", "rep"), "tp"),
        P(("fs", "rep"), "tp"),
        P(("fs", "rep"), "tp"),
        P(None, "tp"),
        P(None, "tp"),
    )
    return jax.shard_map(functools.partial(fused, body), mesh=mesh, in_specs=in_specs, out_specs=out_specs, check_vma=False)
```

```python
import functools
import jax
import jax.numpy as jnp
from jax import lax
from jax.experimental import pallas as pl
from jax.experimental.pallas import tpu as pltpu
from jax.sharding import PartitionSpec as P


def moments(projected, first_old, second_old):
    first_new = 0.9 * first_old + 0.1 * projected
    second_new = 0.99 * second_old + 0.01 * projected * projected
    return (first_new, second_new, first_new / (jnp.sqrt(second_new) + 1e-08))


def finish(whole_dir, basis_rows, weight, squares, entries):
    norm_scale = jnp.sqrt(squares / entries + 1.0)
    update = jnp.dot(basis_rows, whole_dir, precision=lax.Precision.HIGHEST) / norm_scale
    weight_new = weight - 0.01 * update
    return (update, weight_new, weight_new.astype(jnp.bfloat16))


def split_parts(reduced):
    high_part = reduced.astype(jnp.bfloat16)
    held = lax.optimization_barrier(high_part)
    low_part = (reduced - held.astype(jnp.float32)).astype(jnp.bfloat16)
    return (high_part, low_part)


def parts_product(high_part, low_part, cotangent):
    dims = (((0,), (0,)), ((), ()))
    first_term = lax.dot_general(high_part, cotangent, dims, preferred_element_type=jnp.float32)
    second_term = lax.dot_general(low_part, cotangent, dims, preferred_element_type=jnp.float32)
    return first_term + second_term


def body(
    normed_input,
    query_cotangent,
    value_cotangent,
    query_basis,
    value_basis,
    query_weight,
    value_weight,
    query_first,
    query_second,
    value_first,
    value_second,
):
    row_count = query_weight.shape[0]
    query_width = query_cotangent.shape[1]
    offset = lax.axis_index(("fs", "rep")) * row_count
    query_rows = lax.dynamic_slice_in_dim(query_basis, offset, row_count, 0).astype(jnp.float32)
    value_rows = lax.dynamic_slice_in_dim(value_basis, offset, row_count, 0).astype(jnp.float32)
    reduced_query = jnp.dot(normed_input, query_basis, preferred_element_type=jnp.float32)
    reduced_value = jnp.dot(normed_input, value_basis, preferred_element_type=jnp.float32)
    query_high, query_low = split_parts(reduced_query)
    value_high, value_low = split_parts(reduced_value)
    projected = lax.psum_scatter(
        jnp.concatenate(
            [
                parts_product(query_high, query_low, query_cotangent),
                parts_product(value_high, value_low, value_cotangent),
            ],
            axis=1,
        ),
        ("fs", "rep"),
        scatter_dimension=0,
        tiled=True,
    )
    query_projected = projected[:, :query_width]
    value_projected = projected[:, query_width:]
    query_first_new, query_second_new, query_dir = moments(
        query_projected, query_first, query_second
    )
    value_first_new, value_second_new, value_dir = moments(
        value_projected, value_first, value_second
    )
    query_whole, value_whole = (
        lax.all_gather(query_dir, ("fs", "rep"), axis=0, tiled=True),
        lax.all_gather(value_dir, ("fs", "rep"), axis=0, tiled=True),
    )
    query_squares, value_squares = lax.psum(
        (jnp.sum(query_dir * query_dir), jnp.sum(value_dir * value_dir)), ("fs", "rep", "tp")
    )
    tp_count = lax.axis_size("tp")
    query_update, query_weight_new, query_half = finish(
        query_whole,
        query_rows,
        query_weight,
        query_squares,
        query_whole.shape[0] * query_whole.shape[1] * tp_count,
    )
    value_update, value_weight_new, value_half = finish(
        value_whole,
        value_rows,
        value_weight,
        value_squares,
        value_whole.shape[0] * value_whole.shape[1] * tp_count,
    )
    query_copy, value_copy = (
        lax.all_gather(query_half, ("fs", "rep"), axis=0, tiled=True),
        lax.all_gather(value_half, ("fs", "rep"), axis=0, tiled=True),
    )
    return (
        query_update,
        value_update,
        query_weight_new,
        value_weight_new,
        query_first_new,
        query_second_new,
        value_first_new,
        value_second_new,
        query_copy,
        value_copy,
    )


MESH = pl.DeviceIdType.MESH
ORDER = (1, 3, 2)
EARLY_FS = 2
REP_AT = 1
SPLIT_EARLY = True
VMEM_LIMIT = 60 * 2**20
OUT_LIMIT = 16 * 2**20
f32, bf16 = jnp.float32, jnp.bfloat16


def two_parts(x):
    high = x.astype(bf16)
    return high, (x - high.astype(f32)).astype(bf16)


def three_parts(x):
    high = x.astype(bf16)
    rest = x - high.astype(f32)
    middle = rest.astype(bf16)
    return high, middle, (rest - middle.astype(f32)).astype(bf16)


def remote(src, dst, sems, index, peer):
    return pltpu.make_async_remote_copy(
        src_ref=src,
        dst_ref=dst,
        send_sem=sems[0].at[index],
        recv_sem=sems[1].at[index],
        device_id=peer,
        device_id_type=MESH,
    )


def kernel(
    F, R, T,
    x_hbm, qc_hbm, vc_hbm, qb_hbm, vb_hbm, qw_hbm, vw_hbm, qf_hbm, qs_hbm, vf_hbm, vs_hbm,
    u_ref, n_ref, fn_ref, sn_ref, copy_ref,
    x_ref, qc_ref, vc_ref, qb_ref, vb_ref, w_ref, f_ref, s_ref, near_ref,
    part, got1, mid, got2, dirs, squares, squares_in,
    load, s1, r1, s2, r2, s3, r3, s4, r4, s5, r5, s6, r6, s7, r7, s8, r8, s9, r9,
):
    z, r, t = lax.axis_index("fs"), lax.axis_index("rep"), lax.axis_index("tp")
    zs = [lax.rem(z + k, F) for k in range(F)]
    rs = [lax.rem(r + k, R) for k in range(R)]
    ts = [lax.rem(t + k, T) for k in range(T)]
    back = [lax.rem(z + F - k, F) for k in range(F)]
    if F == 4:
        pairs = {1: z + 1 - 2 * lax.rem(z, 2), 2: lax.rem(z + 2, 4), 3: 3 - z}
        zs = back = [z] + [pairs[k] for k in ORDER]
    rows = qw_hbm.shape[0]
    QC, VC = qc_hbm.shape[1], vc_hbm.shape[1]
    M = qf_hbm.shape[0]

    barrier = pltpu.get_barrier_semaphore()
    for axis, others in (("rep", rs), ("fs", zs), ("tp", ts)):
        for other in others[1:]:
            pl.semaphore_signal(barrier, inc=1, device_id={axis: other}, device_id_type=MESH)

    query, value = pl.ds(0, QC), pl.ds(QC, VC)
    loads = [
        pltpu.make_async_copy(src, dst, load.at[i])
        for i, (src, dst) in enumerate((
            (x_hbm, x_ref),
            (qb_hbm, qb_ref),
            (qc_hbm, qc_ref),
            (vb_hbm, vb_ref),
            (vc_hbm, vc_ref),
            (qf_hbm, f_ref.at[:, query]),
            (vf_hbm, f_ref.at[:, value]),
            (qs_hbm, s_ref.at[:, query]),
            (vs_hbm, s_ref.at[:, value]),
            (qw_hbm, w_ref.at[:, query]),
            (vw_hbm, w_ref.at[:, value]),
        ))
    ]
    for c in loads:
        c.start()

    loads[0].wait()
    x = x_ref[...]
    for i, (basis, cot, start, width) in enumerate(
        ((qb_ref, qc_ref, 0, QC), (vb_ref, vc_ref, QC, VC))
    ):
        loads[1 + 2 * i].wait()
        loads[2 + 2 * i].wait()
        reduced = jnp.dot(x, basis[...], preferred_element_type=f32).T
        high, low = two_parts(reduced)
        c = cot[...]
        total = jnp.dot(high, c, preferred_element_type=f32) + jnp.dot(
            low, c, preferred_element_type=f32
        )
        for a in range(F):
            for b in range(R):
                at = (a * R + b) * M
                part[b, a, :, start : start + width] = total[at : at + M]

    pl.semaphore_wait(barrier, F + R + T - 3)

    sends = []
    rback = [lax.rem(r + R - k, R) for k in range(R)]
    reach = min(EARLY_FS, F - 1)
    middle_row = rows // 2 // 8 * 8 if SPLIT_EARLY else rows
    tops = [(0, middle_row)] + ([(middle_row, rows)] if middle_row < rows else [])
    near = {}
    for k in range(1, reach + 1):
        for i, (lo, hi) in enumerate(tops if k > 1 else [(0, rows)]):
            near[k, i] = remote(
                w_ref.at[lo:hi], near_ref.at[k - 1, lo:hi], (s8, r8), 2 * k + i, {"fs": zs[k]}
            )
    near_rep = [
        remote(w_ref, near_ref.at[reach + k - 1], (s9, r9), k, {"rep": rs[k]})
        for k in range(1, R)
        if REP_AT
    ]
    sends += list(near.values()) + near_rep
    order = list(range(1, F)) + [0]
    first = {
        (j, k): remote(
            part.at[rs[k], zs[j]], got1.at[k, j], (s1, r1), (j, k), {"rep": rs[k]}
        )
        for j in order
        for k in range(1, R)
    }
    for c in first.values():
        c.start()
    sends += list(first.values())
    for c in loads[9:]:
        c.wait()
    if REP_AT == 1:
        for c in near_rep:
            c.start()
    for (k, i), c in near.items():
        if i == 0:
            c.start()
    second = {}
    for j in order:
        total = part[r, zs[j]]
        for k in range(1, R):
            first[j, k].wait_recv()
            total = total + got1[k, j]
        if j > 0:
            mid[j] = total
            second[j] = remote(mid.at[j], got2.at[j], (s2, r2), j, {"fs": zs[j]})
            second[j].start()
    sends += list(second.values())
    if REP_AT == 2:
        for c in near_rep:
            c.start()
    for c in loads[5:9]:
        c.wait()
    projected = total
    for j in range(1, F):
        second[j].wait_recv()
        projected = projected + got2[j]

    fn = 0.9 * f_ref[...] + 0.1 * projected
    sn = 0.99 * s_ref[...] + 0.01 * projected * projected
    dirs[z, r] = fn / (jnp.sqrt(sn) + 1e-08)

    third = [remote(dirs.at[z, r], dirs.at[z, r], (s3, r3), k, {"fs": zs[k]}) for k in range(1, F)]
    for c in third:
        c.start()
    for (k, i), c in near.items():
        if i == 1:
            c.start()
    sends += third
    fourth = []
    for j in range(F):
        if j > 0:
            third[j - 1].wait_recv()
        block = dirs.at[back[j], r]
        for k in range(1, R):
            c = remote(block, block, (s4, r4), (j, k), {"rep": rs[k]})
            c.start()
            fourth.append(c)
        if j == 0:
            fn_ref[...] = fn
            sn_ref[...] = sn
    sends += fourth
    for c in fourth:
        c.wait_recv()

    whole = dirs[...].reshape(F * R * M, QC + VC)
    for i, (start, width) in enumerate(((0, QC), (QC, VC))):
        d = whole[:, start : start + width]
        d = (d * d).reshape(F * R * M // 8, 8, width).sum(axis=0)
        acc = d[:, :128]
        for b in range(1, width // 128):
            acc = acc + d[:, b * 128 : (b + 1) * 128]
        squares[i] = acc
    fifth = [remote(squares, squares_in.at[k], (s5, r5), k, {"tp": ts[k]}) for k in range(1, T)]
    for c in fifth:
        c.start()
    sends += fifth

    offset = pl.multiple_of((z * R + r) * rows, rows)
    split_dirs = [three_parts(whole[:, lo : lo + n]) for lo, n in ((0, QC), (QC, VC))]

    def start_of(fs, rep):
        return pl.multiple_of((fs * R + rep) * rows, rows)

    def product(starts):
        results = []
        for basis, (d1, d2, d3) in zip((qb_ref, vb_ref), split_dirs):
            b = jnp.concatenate([basis[pl.ds(at, rows), :] for at in starts], axis=0)
            results.append(
                jnp.dot(b, d1, preferred_element_type=f32)
                + (
                    jnp.dot(b, d2, preferred_element_type=f32)
                    + jnp.dot(b, d3, preferred_element_type=f32)
                )
            )
        return results

    beyond = [start_of(back[k], r) for k in range(1, reach + 1)]
    raw = product([offset] + beyond)
    for c in near.values():
        c.wait_recv()
    for c in fifth:
        c.wait_recv()
    sq = squares[...]
    for k in range(1, T):
        sq = sq + squares_in[k]
    spans = ((0, QC), (QC, VC))
    scales = [
        jnp.sqrt(jnp.sum(sq[i], keepdims=True) / (F * R * M * width * T) + 1.0)
        for i, (start, width) in enumerate(spans)
    ]

    def copy_rows(raw, first, starts, slot):
        for i, (start, width) in enumerate(spans):
            for n, at in enumerate(starts):
                update = raw[i][(first + n) * rows : (first + n + 1) * rows] / scales[i]
                new = near_ref[slot + n, :, start : start + width] - 0.01 * update
                copy_ref[pl.ds(at, rows), start : start + width] = new.astype(bf16)

    for i, (start, width) in enumerate(spans):
        update = raw[i][:rows] / scales[i]
        new = w_ref[:, start : start + width] - 0.01 * update
        copy_ref[pl.ds(offset, rows), start : start + width] = new.astype(bf16)
        u_ref[:, start : start + width] = update
        n_ref[:, start : start + width] = new
    copy_rows(raw, 1, beyond, 0)

    parts = 2 if R == 4 and rows % 32 == 0 else 1
    size = rows // parts

    def piece(j, rep, p):
        at = pl.multiple_of((back[j] * R + rep) * rows + p * size, size)
        return copy_ref.at[pl.ds(at, size), :]

    ready = 1 + reach
    sixth = {}
    for k in range(ready, F):
        for p in range(parts):
            own = piece(0, r, p)
            sixth[k, p] = remote(own, own, (s6, r6), (k, p), {"fs": zs[k]})
            sixth[k, p].start()
    sends += list(sixth.values())

    last = []
    beside = (r + 1 - 2 * lax.rem(r, 2), lax.rem(r + 2, 4))
    direct = {}

    def forward(j):
        for a in range(2):
            direct[j, a, a].wait_recv()
            block = piece(j, beside[a], a)
            c = remote(block, block, (s7, r7), (j, 4 + a), {"rep": beside[1 - a]})
            c.start()
            last.append(c)

    first_block = 1 if REP_AT else 0
    for j in range(first_block, F):
        if REP_AT and j == min(ready, F - 1):
            beside_rows = [start_of(z, rback[k]) for k in range(1, R)]
            raw = product(beside_rows)
            for c in near_rep:
                c.wait_recv()
            copy_rows(raw, 0, beside_rows, reach)
        for p in range(parts):
            if j >= ready:
                sixth[j, p].wait_recv()
            if parts == 1:
                for k in range(1, R):
                    block = piece(j, r, 0)
                    c = remote(block, block, (s7, r7), (j, k), {"rep": rs[k]})
                    c.start()
                    last.append(c)
            elif j >= ready:
                for a in (p, 1 - p):
                    block = piece(j, r, p)
                    direct[j, a, p] = remote(block, block, (s7, r7), (j, a * 2 + p), {"rep": beside[a]})
                    direct[j, a, p].start()
        if parts == 2 and j < ready:
            for a, p in ((0, 0), (1, 1), (0, 1), (1, 0)):
                block = piece(j, r, p)
                direct[j, a, p] = remote(block, block, (s7, r7), (j, a * 2 + p), {"rep": beside[a]})
                direct[j, a, p].start()
        if parts == 2 and j > first_block:
            forward(j - 1)
    if parts == 2:
        forward(F - 1)
    for (j, a, p), c in direct.items():
        if a != p:
            c.wait_recv()
        sends.append(c)
    sends += last
    for c in last:
        c.wait_recv()
    for c in sends:
        c.wait_send()


def write_out(u, n, fn, sn, copy, qu, vu, qn, vn, qfn, qsn, vfn, vsn, qcopy, vcopy, sem):
    QC, VC = qu.shape[1], vu.shape[1]
    query, value = pl.ds(0, QC), pl.ds(QC, VC)
    copies = [
        pltpu.make_async_copy(src.at[:, part], dst, sem.at[i])
        for i, (src, part, dst) in enumerate((
            (copy, value, vcopy),
            (copy, query, qcopy),
            (u, value, vu),
            (n, value, vn),
            (u, query, qu),
            (n, query, qn),
            (fn, query, qfn),
            (fn, value, vfn),
            (sn, query, qsn),
            (sn, value, vsn),
        ))
    ]
    for c in copies:
        c.start()
    for c in copies:
        c.wait()


def fused(plain, *args):
    x, qc, vc, qb, vb, qw, vw, qf, qs, vf, vs = args
    F, R, T = (lax.axis_size(name) for name in ("fs", "rep", "tp"))
    QC, VC = qc.shape[1], vc.shape[1]
    M, rows = qf.shape[0], qw.shape[0]
    aligned = M % 8 == 0 and rows % 16 == 0 and QC % 128 == 0 and VC % 128 == 0
    if not aligned:
        return plain(*args)
    W = QC + VC
    out = jax.ShapeDtypeStruct
    vmem = pl.BlockSpec(memory_space=pltpu.VMEM)
    dma = pltpu.SemaphoreType.DMA
    results = pl.pallas_call(
        functools.partial(kernel, F, R, T),
        out_shape=[
            pltpu.VMEM((rows, W), f32),
            pltpu.VMEM((rows, W), f32),
            pltpu.VMEM((M, W), f32),
            pltpu.VMEM((M, W), f32),
            pltpu.VMEM((rows * F * R, W), bf16),
        ],
        in_specs=[pl.BlockSpec(memory_space=pltpu.HBM)] * 11,
        out_specs=[vmem] * 5,
        scratch_shapes=[
            pltpu.VMEM(x.shape, bf16),
            pltpu.VMEM(qc.shape, bf16),
            pltpu.VMEM(vc.shape, bf16),
            pltpu.VMEM(qb.shape, bf16),
            pltpu.VMEM(vb.shape, bf16),
            pltpu.VMEM((rows, W), f32),
            pltpu.VMEM((M, W), f32),
            pltpu.VMEM((M, W), f32),
            pltpu.VMEM((min(EARLY_FS, F - 1) + R - 1, rows, W), f32),
            pltpu.VMEM((R, F, M, W), f32),
            pltpu.VMEM((R, F, M, W), f32),
            pltpu.VMEM((F, M, W), f32),
            pltpu.VMEM((F, M, W), f32),
            pltpu.VMEM((F, R, M, W), f32),
            pltpu.VMEM((2, 8, 128), f32),
            pltpu.VMEM((T, 2, 8, 128), f32),
            dma((11,)),
            dma((F, R)), dma((F, R)),
            dma((F,)), dma((F,)),
            dma((F,)), dma((F,)),
            dma((F, R)), dma((F, R)),
            dma((T,)), dma((T,)),
            dma((F, 2)), dma((F, 2)),
            dma((F, max(R, 6))), dma((F, max(R, 6))),
            dma((2 * F,)), dma((2 * F,)),
            dma((R,)), dma((R,)),
        ],
        compiler_params=pltpu.CompilerParams(
            collective_id=0, has_side_effects=True, vmem_limit_bytes=VMEM_LIMIT
        ),
    )(*args)
    return tuple(
        pl.pallas_call(
            write_out,
            out_shape=[
                out(qw.shape, f32),
                out(vw.shape, f32),
                out(qw.shape, f32),
                out(vw.shape, f32),
                out(qf.shape, f32),
                out(qf.shape, f32),
                out(vf.shape, f32),
                out(vf.shape, f32),
                out((rows * F * R, QC), bf16),
                out((rows * F * R, VC), bf16),
            ],
            in_specs=[vmem] * 5,
            out_specs=[pl.BlockSpec(memory_space=pltpu.HBM)] * 10,
            scratch_shapes=[dma((10,))],
            compiler_params=pltpu.CompilerParams(vmem_limit_bytes=OUT_LIMIT),
        )(*results)
    )


def solution(mesh):
    in_specs = (
        P(("fs", "rep"), None),
        P(("fs", "rep"), "tp"),
        P(("fs", "rep"), "tp"),
        P(),
        P(),
        P(("fs", "rep"), "tp"),
        P(("fs", "rep"), "tp"),
        P(("fs", "rep"), "tp"),
        P(("fs", "rep"), "tp"),
        P(("fs", "rep"), "tp"),
        P(("fs", "rep"), "tp"),
    )
    out_specs = (
        P(("fs", "rep"), "tp"),
        P(("fs", "rep"), "tp"),
        P(("fs", "rep"), "tp"),
        P(("fs", "rep"), "tp"),
        P(("fs", "rep"), "tp"),
        P(("fs", "rep"), "tp"),
        P(("fs", "rep"), "tp"),
        P(("fs", "rep"), "tp"),
        P(None, "tp"),
        P(None, "tp"),
    )
    return jax.shard_map(functools.partial(fused, body), mesh=mesh, in_specs=in_specs, out_specs=out_specs, check_vma=False)
```
